32 devices in a mesh: grp: 2 (over y), tp: 4 (over z), dp: 4 (over x, core).
Axes of the slice: x: 2, y: 2, z: 4, core: 2. Of those that a mesh axis runs over, the one named last changes fastest.
Arguments:
- tokens: bfloat16 [128, 4096], P('grp', 'dp'), parts along dimension 0, may hold values from -50 to 50
- lengths: int32 [128], P(('grp', 'dp')), parts along dimension 0, may hold values from 1 to 24, as said below
- norm_gain: float32 [2, 4096], P(None, 'dp'), may hold values from 0.1 to 1.9
- w_z: bfloat16 [2, 4096, 4096], P(None, 'dp', 'tp'), may hold values from -0.09375 to 0.09375
- w_x: bfloat16 [2, 4096, 4096], P(None, 'dp', 'tp'), may hold values from -0.09375 to 0.09375
- w_b: bfloat16 [2, 4096, 2048], P(None, 'dp', 'tp'), may hold values from -0.09375 to 0.09375
- w_c: bfloat16 [2, 4096, 2048], P(None, 'dp', 'tp'), may hold values from -0.09375 to 0.09375
- w_dt: bfloat16 [2, 4096, 64], P(None, 'dp'), may hold values from -0.09375 to 0.09375
- conv_weight: bfloat16 [2, 4, 8192], P(None, None, 'tp'), may hold values from -3 to 3
- dt_bias: float32 [2, 64], P(None, 'tp'), may hold values from -6 to -1.5
- a_log: float32 [2, 64], P(None, 'tp'), may hold values from 0 to 2.77
- d_skip: float32 [2, 64], P(None, 'tp'), may hold values from 0.1 to 1.9
- out_gain: float32 [2, 4096], P(None, 'tp'), may hold values from 0.1 to 1.9
- w_out: bfloat16 [2, 4096, 4096], P(None, 'tp', 'dp'), may hold values from -0.09375 to 0.09375
- conv_state: bfloat16 [2, 128, 3, 8192], P(None, ('grp', 'dp'), None, 'tp'), parts along dimension 1, may hold values from -6 to 6
- ssm_state: float32 [2, 128, 64, 64, 128], P(None, ('grp', 'dp'), 'tp'), parts along dimension 1, may hold values from -2 to 2
Outputs:
- mixed_out: bfloat16 [128, 4096], P('grp', 'dp'), parts along dimension 0
- conv_new: bfloat16 [2, 128, 3, 8192], P(None, ('grp', 'dp'), None, 'tp'), parts along dimension 1
- ssm_new: float32 [2, 128, 64, 64, 128], P(None, ('grp', 'dp'), 'tp'), parts along dimension 1
The draws below stay inside these ranges and needn't reach their ends.
There are 2 independent parts, one for each index of `grp`. The reference program is written for one: setup_inputs(seed, part) draws one part's arguments, and reference() takes and returns one part's arrays. A program takes and returns all parts, laid end to end along the dimension named above; an argument that names none is the same for every part. Nothing has to cross between parts.
Inputs may be any that keep to these rules, and one draw needn't show every extreme that they name: `lengths`: each part has at least one sequence of length 24.
All inputs are finite; a program needn't handle non-finite values.
Results may differ from the reference program's by a relative error of at most 0.012.
Values may be sent and summed in bfloat16 or wider, within the bound.
A program may use at most 128 MiB of HBM per device.

```python
import jax
import jax.numpy as jnp
from jax import lax

D = 4096
HEADS = 64
GROUPS = 16
HEAD_DIM = 64
STATE = 128
CONV_W = 4
LAYERS = 2
BATCH = 64
SSD_W = 4096
CONV_DIM = 8192


def draw_tokens(key, part):
    first_key = jax.random.fold_in(key, 11)
    second_key = jax.random.fold_in(key, 12)
    columns = 10.0 ** (jnp.arange(D, dtype=jnp.float32) / D - 0.5)
    rowscale = jnp.exp(jax.random.uniform(first_key, (BATCH,), jnp.float32, -1.1513, 1.1513))
    entries = jnp.clip(jax.random.normal(second_key, (BATCH, D), jnp.float32), -5.0, 5.0)
    return (entries * rowscale[:, None] * columns[None, :]).astype(jnp.bfloat16)


def draw_lengths(key, part):
    short_key = jax.random.fold_in(key, 21)
    pick_key = jax.random.fold_in(key, 22)
    long_key = jax.random.fold_in(key, 23)
    place_key = jax.random.fold_in(key, 24)
    short_len = jax.random.randint(short_key, (BATCH,), 1, 7, dtype=jnp.int32)
    picked = jax.random.randint(pick_key, (BATCH,), 0, 8, dtype=jnp.int32) == 0
    long_len = jax.random.randint(long_key, (BATCH,), 12, 25, dtype=jnp.int32)
    chosen = jnp.where(picked, long_len, short_len)
    place = jax.random.randint(place_key, (), 0, BATCH, dtype=jnp.int32)
    return jnp.where(jnp.arange(BATCH, dtype=jnp.int32) == place, jnp.int32(24), chosen).astype(jnp.int32)


def block_scale(rng, dims, cuts, smallest, top_value):
    def one(dim, blocks):
        heights = jax.random.uniform(jax.random.fold_in(jax.random.fold_in(rng, 6), dim), (blocks,), jnp.float32, smallest / len(cuts), top_value / len(cuts))
        return jnp.repeat(jnp.exp(heights), dims[dim] // blocks).reshape((-1,) + (1,) * (len(dims) - dim - 1))

    factor_of = one(*cuts[0])
    for cut in cuts[1:]:
        factor_of = factor_of * one(*cut)
    return factor_of


def bell_draw(stream_key, shape, spread, limit, cuts=(), kind=jnp.bfloat16):
    drawn = spread * jax.random.normal(stream_key, shape, jnp.float32)
    if cuts:
        drawn = drawn * block_scale(stream_key, shape, cuts, -0.22, 0.18)
    return jnp.clip(drawn, -limit, limit).astype(kind)


def setup_inputs(seed: int = 0, part: int = 0) -> dict:
    arg_keys = jax.random.split(jax.random.key(seed), 17)
    own_keys = jax.random.split(jax.random.fold_in(arg_keys[16], part), 17)
    return {
        "tokens": draw_tokens(jax.random.fold_in(jax.random.fold_in(arg_keys[16], part), 71), part),
        "lengths": draw_lengths(jax.random.fold_in(jax.random.fold_in(arg_keys[16], part), 71), part),
        "norm_gain": jnp.clip(1.0 + 0.18 * jax.random.normal(arg_keys[2], (LAYERS, D), jnp.float32), 0.1, 1.9),
        "w_z": bell_draw(arg_keys[3], (LAYERS, D, SSD_W), D ** -0.5, 0.09375, ((1, 4), (2, 4))),
        "w_x": bell_draw(arg_keys[4], (LAYERS, D, SSD_W), D ** -0.5, 0.09375, ((1, 4), (2, 4))),
        "w_b": bell_draw(arg_keys[5], (LAYERS, D, GROUPS * STATE), D ** -0.5, 0.09375, ((1, 4), (2, 4))),
        "w_c": bell_draw(arg_keys[6], (LAYERS, D, GROUPS * STATE), D ** -0.5, 0.09375, ((1, 4), (2, 4))),
        "w_dt": bell_draw(arg_keys[7], (LAYERS, D, HEADS), D ** -0.5, 0.09375, ((1, 4),)),
        "conv_weight": bell_draw(arg_keys[8], (LAYERS, CONV_W, CONV_DIM), 0.5, 3.0, ((2, 4),)),
        "dt_bias": jnp.clip(-6.0 + 4.5 * jax.random.uniform(arg_keys[9], (LAYERS, HEADS), jnp.float32) ** block_scale(arg_keys[9], (LAYERS, HEADS), ((1, 4),), -0.2, 0.2), -6.0, -1.5),
        "a_log": jnp.clip(2.77 * jax.random.uniform(arg_keys[10], (LAYERS, HEADS), jnp.float32) ** block_scale(arg_keys[10], (LAYERS, HEADS), ((1, 4),), -0.2, 0.2), 0.0, 2.77),
        "d_skip": jnp.clip(1.0 + 0.18 * jax.random.normal(arg_keys[11], (LAYERS, HEADS), jnp.float32), 0.1, 1.9),
        "out_gain": jnp.clip(1.0 + 0.18 * jax.random.normal(arg_keys[12], (LAYERS, SSD_W), jnp.float32), 0.1, 1.9),
        "w_out": bell_draw(arg_keys[13], (LAYERS, SSD_W, D), SSD_W ** -0.5, 0.09375, ((1, 4), (2, 4))),
        "conv_state": bell_draw(own_keys[14], (LAYERS, BATCH, CONV_W - 1, CONV_DIM), 1.0, 6.0, ((1, 4), (3, 4))),
        "ssm_state": bell_draw(own_keys[15], (LAYERS, BATCH, HEADS, HEAD_DIM, STATE), 0.15, 2.0, ((1, 4), (2, 4)), jnp.float32),
    }


EPSILON = 1e-06

def one_block(stream, lengths, gain, w_z, w_x, w_b, w_c, w_dt, taps_weight, dt_bias, a_log, d_skip, out_gain, w_out, conv_past, ssm_past):
    batch_rows = stream.shape[0]
    per_group = HEADS // GROUPS
    width_x = per_group * HEAD_DIM
    wide = stream.astype(jnp.float32)
    inverse = lax.rsqrt(lax.optimization_barrier(jnp.mean(wide * wide, axis=-1)) + EPSILON)[:, None]
    normed = (wide * gain).astype(jnp.bfloat16)
    gating = (jnp.dot(normed, w_z, preferred_element_type=jnp.float32) * inverse).astype(jnp.bfloat16)
    values = (jnp.dot(normed, w_x, preferred_element_type=jnp.float32) * inverse).astype(jnp.bfloat16)
    writes = (jnp.dot(normed, w_b, preferred_element_type=jnp.float32) * inverse).astype(jnp.bfloat16)
    reads = (jnp.dot(normed, w_c, preferred_element_type=jnp.float32) * inverse).astype(jnp.bfloat16)
    step_raw = jnp.dot(normed, w_dt, preferred_element_type=jnp.float32) * inverse
    current = jnp.concatenate([values.reshape(batch_rows, GROUPS, width_x), writes.reshape(batch_rows, GROUPS, STATE), reads.reshape(batch_rows, GROUPS, STATE)], axis=-1).reshape(batch_rows, CONV_DIM)
    offsets = jnp.arange(CONV_W - 1, dtype=jnp.int32)
    alive = lengths[:, None] + offsets[None, :] >= CONV_W
    history = jnp.where(alive[:, :, None], conv_past, jnp.zeros_like(conv_past))
    conv_next = jnp.concatenate([history[:, 1:], current[:, None]], axis=1)
    summed = current.astype(jnp.float32) * taps_weight[CONV_W - 1].astype(jnp.float32)
    for tap_at in range(CONV_W - 1):
        summed = summed + history[:, tap_at].astype(jnp.float32) * taps_weight[tap_at].astype(jnp.float32)
    activated = jax.nn.silu(summed).reshape(batch_rows, GROUPS, width_x + 2 * STATE)
    head_in = activated[:, :, :width_x].reshape(batch_rows, GROUPS, per_group, HEAD_DIM)
    write_keys = activated[:, :, width_x:width_x + STATE]
    read_keys = activated[:, :, width_x + STATE:]
    step = jax.nn.softplus(step_raw + dt_bias).reshape(batch_rows, GROUPS, per_group)
    decay = jnp.exp(-jnp.exp(a_log).reshape(GROUPS, per_group) * step)
    carried = lengths >= 2
    before = ssm_past.reshape(batch_rows, GROUPS, per_group, HEAD_DIM, STATE)
    before = jnp.where(carried[:, None, None, None, None], before, jnp.zeros_like(before))
    state_next = decay[..., None, None] * before + (step[..., None] * head_in)[..., None] * write_keys[:, :, None, None, :]
    readout = jnp.einsum('bghpn,bgn->bghp', state_next, read_keys, precision=lax.Precision.HIGHEST)
    readout = readout + d_skip.reshape(GROUPS, per_group)[..., None] * head_in
    gated = readout.reshape(batch_rows, GROUPS, width_x) * jax.nn.silu(gating.astype(jnp.float32).reshape(batch_rows, GROUPS, width_x))
    gated = gated * lax.rsqrt(lax.optimization_barrier(jnp.mean(gated * gated, axis=-1, keepdims=True)) + EPSILON) * out_gain.reshape(GROUPS, width_x)
    mixed = gated.reshape(batch_rows, SSD_W).astype(jnp.bfloat16)
    stream_next = (wide + jnp.dot(mixed, w_out, preferred_element_type=jnp.float32)).astype(jnp.bfloat16)
    return (stream_next, conv_next, state_next.reshape(batch_rows, HEADS, HEAD_DIM, STATE))

def reference(tokens, lengths, norm_gain, w_z, w_x, w_b, w_c, w_dt, conv_weight, dt_bias, a_log, d_skip, out_gain, w_out, conv_state, ssm_state):
    stream = tokens
    conv_list = []
    ssm_list = []
    for layer_at in range(LAYERS):
        stream, conv_next, state_next = one_block(stream, lengths, norm_gain[layer_at], w_z[layer_at], w_x[layer_at], w_b[layer_at], w_c[layer_at], w_dt[layer_at], conv_weight[layer_at], dt_bias[layer_at], a_log[layer_at], d_skip[layer_at], out_gain[layer_at], w_out[layer_at], conv_state[layer_at], ssm_state[layer_at])
        conv_list.append(conv_next)
        ssm_list.append(state_next)
    return (stream, jnp.stack(conv_list), jnp.stack(ssm_list))
```

```python
import functools

import jax
import jax.numpy as jnp
from jax import lax
from jax.experimental import pallas as pl
from jax.experimental.pallas import tpu as pltpu
from jax.sharding import PartitionSpec as P

D = 4096
HEADS = 64
GROUPS = 16
HEAD_DIM = 64
STATE = 128
CONV_W = 4
PER_GROUP = HEADS // GROUPS
WIDTH_X = PER_GROUP * HEAD_DIM
GROUP_W = WIDTH_X + 2 * STATE
EPSILON = 1e-06
MESH = pl.DeviceIdType.MESH
BF16 = jnp.bfloat16
F32 = jnp.float32


def silu(t):
    return t / (1.0 + jnp.exp(-t))


def block_kernel(
    nd, nt,
    tokens_ref, lens_ref, gain_ref, bias_ref, alog_ref, skip_ref, ogain_ref, taps_ref, conv_ref,
    wz_hbm, wx_hbm, wb_hbm, wc_hbm, wdt_hbm, wo_hbm, state_hbm,
    out_ref, cur_ref, dec_ref, sx_ref, wk_ref,
    wz, wx, wb, wc, wdt, wo, state,
    snd_e, snd_x, snd_b, snd_c, snd_z,
    rcv_e, rcv_x, rcv_b, rcv_c, rcv_z,
    mixes, snd_o, rcv_o, stream, normed_s, rk_s, y_s,
    w_sem, st_sem, dps, dpr, ags, agr, rss, rsr, tgs, tgr,
):
    dp = lax.axis_index("dp")
    tp = lax.axis_index("tp")
    layers = gain_ref.shape[0]
    seqs = lens_ref.shape[0]
    batch = nd * seqs
    rows = batch // nt
    dloc = gain_ref.shape[1]
    width = wx.shape[2]
    lgroups = width // WIDTH_X

    pairs = ((wdt_hbm, wdt), (wx_hbm, wx), (wb_hbm, wb), (wc_hbm, wc), (wz_hbm, wz), (wo_hbm, wo))

    def weight(layer, at):
        src, dst = pairs[at]
        return pltpu.make_async_copy(src.at[layer], dst.at[layer], w_sem.at[layer, at])

    def states(layer):
        return pltpu.make_async_copy(state_hbm.at[layer], state.at[layer], st_sem.at[layer])

    for at in range(5):
        weight(0, at).start()

    barrier = pltpu.get_barrier_semaphore()
    for k in range(1, nd):
        pl.semaphore_signal(
            barrier, inc=1, device_id={"dp": lax.rem(dp + k, nd)}, device_id_type=MESH
        )
    for k in range(1, nt):
        pl.semaphore_signal(
            barrier, inc=1, device_id={"tp": lax.rem(tp + k, nt)}, device_id_type=MESH
        )
    pl.semaphore_wait(barrier, nd - 1 + nt - 1)

    def scatter(layer, snd, rcv, at):
        copies = []
        for k in range(1, nd):
            peer = lax.rem(dp + k, nd)
            copy = pltpu.make_async_remote_copy(
                src_ref=snd.at[layer, peer],
                dst_ref=rcv.at[layer, k - 1],
                send_sem=dps.at[layer, at, k - 1],
                recv_sem=dpr.at[layer, at, k - 1],
                device_id={"dp": peer},
                device_id_type=MESH,
            )
            copy.start()
            copies.append(copy)
        return copies

    def gathered(copies, layer, snd, rcv):
        for copy in copies:
            copy.wait_recv()
        total = snd[layer, dp].astype(F32)
        for k in range(nd - 1):
            total = total + rcv[layer, k].astype(F32)
        return total

    heads_all = wdt.shape[2]
    lheads = bias_ref.shape[1]

    def expand(values, offset):
        count = values.shape[1]
        head = lax.broadcasted_iota(jnp.int32, (count, width), 0)
        lane = lax.broadcasted_iota(jnp.int32, (count, width), 1)
        pick = jnp.where(head == lane // HEAD_DIM + offset, 1.0, 0.0).astype(F32)
        return jnp.dot(
            values, pick, preferred_element_type=F32, precision=lax.Precision.HIGHEST
        )

    bias = expand(bias_ref[...], 0)
    rate = jnp.exp(expand(alog_ref[...], 0))
    skip = expand(skip_ref[...], 0)
    lens = lens_ref[...]
    pending = []

    for layer in range(layers):
        source = tokens_ref if layer == 0 else stream.at[layer - 1]
        wide = source[...].astype(F32).reshape(batch, dloc)
        squares = jnp.sum(wide * wide, axis=-1, keepdims=True)
        normed_s[...] = (wide * gain_ref[layer : layer + 1, :]).astype(BF16)

        def project(w_ref, snd, layer=layer):
            n = w_ref.shape[2]
            tile = min(n, 256)

            def step(j, carry):
                cols = pl.ds(pl.multiple_of(j * tile, tile), tile)
                part = jnp.dot(
                    normed_s[...], w_ref[layer, :, cols], preferred_element_type=F32
                )
                snd[layer, :, :, cols] = part.reshape(nd, seqs, tile).astype(snd.dtype)
                return carry

            lax.fori_loop(0, n // tile, step, 0)

        weight(layer, 0).wait()
        part_dt = jnp.dot(normed_s[...], wdt[layer], preferred_element_type=F32)
        snd_e[layer, :, :, 0:128] = jnp.zeros((nd, seqs, 128), F32)
        snd_e[layer, :, :, 0:heads_all] = part_dt.reshape(nd, seqs, heads_all)
        snd_e[layer, :, :, 128:256] = jnp.broadcast_to(squares, (batch, 128)).reshape(
            nd, seqs, 128
        )
        weight(layer, 1).wait()
        project(wx, snd_x)
        copies_x = scatter(layer, snd_x, rcv_x, 1)
        copies_e = scatter(layer, snd_e, rcv_e, 0)
        weight(layer, 2).wait()
        project(wb, snd_b)
        copies_b = scatter(layer, snd_b, rcv_b, 2)
        weight(layer, 3).wait()
        project(wc, snd_c)
        copies_c = scatter(layer, snd_c, rcv_c, 3)
        weight(layer, 4).wait()
        if layer == 0:
            states(0).start()
            weight(0, 5).start()
        project(wz, snd_z)
        copies_z = scatter(layer, snd_z, rcv_z, 4)
        if layer + 1 < layers:
            for at in range(6):
                weight(layer + 1, at).start()
            states(layer + 1).start()

        extra = gathered(copies_e, layer, snd_e, rcv_e)
        inverse = lax.rsqrt(extra[:, 128:129] / D + EPSILON)
        raw = expand(extra[:, 0:heads_all] * inverse, tp * lheads)
        softin = raw + bias[layer : layer + 1, :]
        step = jnp.maximum(softin, 0.0) + jnp.log1p(jnp.exp(-jnp.abs(softin)))
        decay = jnp.exp(-rate[layer : layer + 1, :] * step)
        decay = jnp.where(lens >= 2, decay, 0.0)

        values = (gathered(copies_x, layer, snd_x, rcv_x) * inverse).astype(BF16)
        writes = (gathered(copies_b, layer, snd_b, rcv_b) * inverse).astype(BF16)
        reads = (gathered(copies_c, layer, snd_c, rcv_c) * inverse).astype(BF16)
        pieces = []
        for g in range(lgroups):
            pieces.append(values[:, g * WIDTH_X : (g + 1) * WIDTH_X])
            pieces.append(writes[:, g * STATE : (g + 1) * STATE])
            pieces.append(reads[:, g * STATE : (g + 1) * STATE])
        current = jnp.concatenate(pieces, axis=1)
        cur_ref[layer] = current
        conv_w = lgroups * GROUP_W
        summed = current.astype(F32) * taps_ref[
            layer, CONV_W - 1 : CONV_W, :
        ].astype(F32)
        for tap in range(CONV_W - 1):
            past = conv_ref[layer, :, tap * conv_w : (tap + 1) * conv_w].astype(F32)
            past = jnp.where(lens + tap >= CONV_W, past, 0.0)
            summed = summed + past * taps_ref[layer, tap : tap + 1, :].astype(F32)
        active = silu(summed)
        head_in = jnp.concatenate(
            [active[:, g * GROUP_W : g * GROUP_W + WIDTH_X] for g in range(lgroups)], axis=1
        )
        wk = [
            active[:, g * GROUP_W + WIDTH_X : g * GROUP_W + WIDTH_X + STATE]
            for g in range(lgroups)
        ]
        rk = [active[:, g * GROUP_W + WIDTH_X + STATE : (g + 1) * GROUP_W] for g in range(lgroups)]
        stepx = step * head_in
        dec_ref[layer] = decay
        sx_ref[layer] = stepx
        wk_ref[layer] = jnp.concatenate(wk, axis=1)
        rk_s[...] = jnp.concatenate(rk, axis=1)

        states(layer).wait()

        def read_eight(b, carry, layer=layer):
            at = pl.ds(pl.multiple_of(b * 8, 8), 8)
            keys = rk_s[at, :]
            lines = []
            for i in range(8):
                outs = []
                for g in range(lgroups):
                    row = keys[i : i + 1, g * STATE : (g + 1) * STATE]
                    lhs = jnp.broadcast_to(row, (16, STATE)).astype(BF16)
                    held = state[layer, b * 8 + i, g * PER_GROUP : (g + 1) * PER_GROUP]
                    held = held.reshape(WIDTH_X, STATE).astype(BF16)
                    res = lax.dot_general(
                        lhs, held, (((1,), (1,)), ((), ())), preferred_element_type=F32
                    )
                    outs.append(res[0:1])
                lines.append(jnp.concatenate(outs, axis=1))
            y_s[at, :] = jnp.concatenate(lines, axis=0)
            return carry

        lax.fori_loop(0, seqs // 8, read_eight, 0)
        readout = decay * y_s[...] + skip[layer : layer + 1, :] * head_in
        gate = (gathered(copies_z, layer, snd_z, rcv_z) * inverse).astype(BF16).astype(F32)
        gate = silu(gate)
        mixed = []
        for g in range(lgroups):
            cols = slice(g * WIDTH_X, (g + 1) * WIDTH_X)
            cross = jnp.sum(wk[g] * rk[g], axis=-1, keepdims=True)
            gated = (readout[:, cols] + stepx[:, cols] * cross) * gate[:, cols]
            norm = lax.rsqrt(jnp.mean(gated * gated, axis=-1, keepdims=True) + EPSILON)
            mixed.append(gated * norm * ogain_ref[layer : layer + 1, cols])
        mixes[layer, dp] = jnp.concatenate(mixed, axis=1).astype(BF16)
        copies_m = []
        for k in range(1, nd):
            copy = pltpu.make_async_remote_copy(
                src_ref=mixes.at[layer, dp],
                dst_ref=mixes.at[layer, dp],
                send_sem=ags.at[layer, k - 1],
                recv_sem=agr.at[layer, k - 1],
                device_id={"dp": lax.rem(dp + k, nd)},
                device_id_type=MESH,
            )
            copy.start()
            copies_m.append(copy)
        weight(layer, 5).wait()
        for copy in copies_m:
            copy.wait_recv()

        tile = min(dloc, 256)

        def project_out(j, carry, layer=layer):
            cols = pl.ds(pl.multiple_of(j * tile, tile), tile)
            lhs = mixes[layer].reshape(batch, width)
            part = jnp.dot(lhs, wo[layer, :, cols], preferred_element_type=F32)
            snd_o[layer, :, :, cols] = part.reshape(nt, rows, tile).astype(BF16)
            return carry

        lax.fori_loop(0, dloc // tile, project_out, 0)
        copies_o = []
        for k in range(1, nt):
            peer = lax.rem(tp + k, nt)
            copy = pltpu.make_async_remote_copy(
                src_ref=snd_o.at[layer, peer],
                dst_ref=rcv_o.at[layer, k - 1],
                send_sem=rss.at[layer, k - 1],
                recv_sem=rsr.at[layer, k - 1],
                device_id={"tp": peer},
                device_id_type=MESH,
            )
            copy.start()
            copies_o.append(copy)
        total = source[tp].astype(F32) + snd_o[layer, tp].astype(F32)
        for k in range(nt - 1):
            copies_o[k].wait_recv()
            total = total + rcv_o[layer, k].astype(F32)
        stream[layer, tp] = total.astype(BF16)
        copies_s = []
        for k in range(1, nt):
            copy = pltpu.make_async_remote_copy(
                src_ref=stream.at[layer, tp],
                dst_ref=stream.at[layer, tp],
                send_sem=tgs.at[layer, k - 1],
                recv_sem=tgr.at[layer, k - 1],
                device_id={"tp": lax.rem(tp + k, nt)},
                device_id_type=MESH,
            )
            copy.start()
            copies_s.append(copy)
        for copy in copies_s:
            copy.wait_recv()
        for group in (copies_e, copies_x, copies_b, copies_c, copies_z, copies_m, copies_o, copies_s):
            pending.extend(group)

    out_ref[...] = stream[layers - 1]
    for copy in pending:
        copy.wait_send()


def state_kernel(dec_ref, sx_ref, wk_ref, state_ref, new_ref):
    count = state_ref.shape[1]
    first = pl.program_id(1) * count
    width = dec_ref.shape[2]
    at = pl.ds(pl.multiple_of(first // 8 * 8, 8), 8)
    layer = pl.program_id(0)
    place = lax.rem(first, 8)

    def rows_of(ref):
        block = ref[layer, at, :]
        rows = block[0:count]
        for j in range(count, 8, count):
            rows = jnp.where(place == j, block[j : j + count], rows)
        return rows

    decs, sxs, wks = rows_of(dec_ref), rows_of(sx_ref), rows_of(wk_ref)
    for i in range(count):
        dec = jnp.broadcast_to(decs[i : i + 1], (64, width))
        sx = jnp.broadcast_to(sxs[i : i + 1], (64, width))
        cols = jnp.concatenate([dec, sx], axis=0).T
        for g in range(width // WIDTH_X):
            part = cols[g * WIDTH_X : (g + 1) * WIDTH_X]
            held = state_ref[0, i, g * PER_GROUP : (g + 1) * PER_GROUP].reshape(WIDTH_X, STATE)
            write = wks[i : i + 1, g * STATE : (g + 1) * STATE]
            new = part[:, 0:1] * held + part[:, 64:65] * write
            new_ref[0, i, g * PER_GROUP : (g + 1) * PER_GROUP] = new.reshape(
                PER_GROUP, HEAD_DIM, STATE
            )


def body(
    nd, nt,
    tokens, lengths, norm_gain, w_z, w_x, w_b, w_c, w_dt, conv_weight,
    dt_bias, a_log, d_skip, out_gain, w_out, conv_state, ssm_state,
):
    layers = w_z.shape[0]
    batch, dloc = tokens.shape
    seqs = lengths.shape[0]
    rows = batch // nt
    width = w_x.shape[2]
    keys = w_b.shape[2]
    heads_all = w_dt.shape[2]
    conv_w = conv_weight.shape[2]
    vmem = pl.BlockSpec(memory_space=pltpu.VMEM)
    anywhere = pl.BlockSpec(memory_space=pl.ANY)
    dma = pltpu.SemaphoreType.DMA
    sizes = (width, keys, keys, width)
    stream, current, dec, sx, wk = pl.pallas_call(
        functools.partial(block_kernel, nd, nt),
        out_shape=(
            jax.ShapeDtypeStruct((nt, rows, dloc), BF16),
            jax.ShapeDtypeStruct((layers, seqs, conv_w), BF16),
            jax.ShapeDtypeStruct((layers, seqs, width), F32),
            jax.ShapeDtypeStruct((layers, seqs, width), F32),
            jax.ShapeDtypeStruct((layers, seqs, keys), F32),
        ),
        in_specs=[vmem] * 9 + [anywhere] * 7,
        out_specs=[vmem] * 5,
        scratch_shapes=[
            pltpu.VMEM(w_z.shape, BF16),
            pltpu.VMEM(w_x.shape, BF16),
            pltpu.VMEM(w_b.shape, BF16),
            pltpu.VMEM(w_c.shape, BF16),
            pltpu.VMEM(w_dt.shape, BF16),
            pltpu.VMEM(w_out.shape, BF16),
            pltpu.VMEM(ssm_state.shape, F32),
            pltpu.VMEM((layers, nd, seqs, 256), F32),
            *[pltpu.VMEM((layers, nd, seqs, n), BF16) for n in sizes],
            pltpu.VMEM((layers, nd - 1, seqs, 256), F32),
            *[pltpu.VMEM((layers, nd - 1, seqs, n), BF16) for n in sizes],
            pltpu.VMEM((layers, nd, seqs, width), BF16),
            pltpu.VMEM((layers, nt, rows, dloc), BF16),
            pltpu.VMEM((layers, nt - 1, rows, dloc), BF16),
            pltpu.VMEM((layers, nt, rows, dloc), BF16),
            pltpu.VMEM((batch, dloc), BF16),
            pltpu.VMEM((seqs, keys), F32),
            pltpu.VMEM((seqs, width), F32),
            dma((layers, 6)),
            dma((layers,)),
            dma((layers, 5, nd - 1)),
            dma((layers, 5, nd - 1)),
            dma((layers, nd - 1)),
            dma((layers, nd - 1)),
            dma((layers, nt - 1)),
            dma((layers, nt - 1)),
            dma((layers, nt - 1)),
            dma((layers, nt - 1)),
        ],
        compiler_params=pltpu.CompilerParams(
            collective_id=0, has_side_effects=True, vmem_limit_bytes=56 * 1024 * 1024
        ),
    )(
        tokens.reshape(nt, rows, dloc), lengths[:, None], norm_gain, dt_bias, a_log, d_skip,
        out_gain, conv_weight, conv_state.reshape(layers, seqs, (CONV_W - 1) * conv_w),
        w_z, w_x, w_b, w_c, w_dt, w_out, ssm_state,
    )
    offsets = jnp.arange(1, CONV_W - 1, dtype=jnp.int32)
    alive = lengths[:, None] + offsets[None, :] >= CONV_W
    kept = jnp.where(alive[None, :, :, None], conv_state[:, :, 1:], jnp.zeros((), BF16))
    conv_new = jnp.concatenate([kept, current[:, :, None]], axis=2)
    step = 2
    block = (1, step) + ssm_state.shape[2:]
    ssm_new = pl.pallas_call(
        state_kernel,
        grid=(layers, seqs // step),
        out_shape=jax.ShapeDtypeStruct(ssm_state.shape, F32),
        in_specs=[vmem, vmem, vmem, pl.BlockSpec(block, lambda l, s: (l, s, 0, 0, 0))],
        out_specs=pl.BlockSpec(block, lambda l, s: (l, s, 0, 0, 0)),
    )(dec, sx, wk, ssm_state)
    return stream.reshape(batch, dloc), conv_new, ssm_new


def solution(mesh):
    placed = (
        P("grp", "dp"),
        P(("grp", "dp")),
        P(None, "dp"),
        P(None, "dp", "tp"),
        P(None, "dp", "tp"),
        P(None, "dp", "tp"),
        P(None, "dp", "tp"),
        P(None, "dp", None),
        P(None, None, "tp"),
        P(None, "tp"),
        P(None, "tp"),
        P(None, "tp"),
        P(None, "tp"),
        P(None, "tp", "dp"),
        P(None, ("grp", "dp"), None, "tp"),
        P(None, ("grp", "dp"), "tp", None, None),
    )
    return jax.shard_map(
        functools.partial(body, mesh.shape["dp"], mesh.shape["tp"]),
        mesh=mesh,
        in_specs=placed,
        out_specs=(
            P("grp", "dp"),
            P(None, ("grp", "dp"), None, "tp"),
            P(None, ("grp", "dp"), "tp", None, None),
        ),
        check_vma=False,
    )
```

```python
import functools

import jax
import jax.numpy as jnp
from jax import lax
from jax.experimental import pallas as pl
from jax.experimental.pallas import tpu as pltpu
from jax.sharding import PartitionSpec as P

D = 4096
HEADS = 64
GROUPS = 16
HEAD_DIM = 64
STATE = 128
CONV_W = 4
PER_GROUP = HEADS // GROUPS
WIDTH_X = PER_GROUP * HEAD_DIM
GROUP_W = WIDTH_X + 2 * STATE
EPSILON = 1e-06
MESH = pl.DeviceIdType.MESH
BF16 = jnp.bfloat16
F32 = jnp.float32


def silu(t):
    return t / (1.0 + jnp.exp(-t))


def block_kernel(
    nd, nt,
    tokens_ref, lens_ref, gain_ref, bias_ref, alog_ref, skip_ref, ogain_ref, taps_ref, conv_ref,
    wz_hbm, wx_hbm, wb_hbm, wc_hbm, wdt_hbm, wo_hbm, state_hbm,
    out_ref, cur_ref, kept_ref, dec_ref, sx_ref, wk_ref,
    wz, wx, wb, wc, wdt, wo, state,
    snd_e, snd_x, snd_b, snd_c, snd_z,
    rcv_e, rcv_x, rcv_b, rcv_c, rcv_z,
    mixes, snd_o, rcv_o, stream, normed_s, rk_s, y_s,
    w_sem, st_sem, dps, dpr, ags, agr, rss, rsr, tgs, tgr,
):
    dp = lax.axis_index("dp")
    tp = lax.axis_index("tp")
    layers = gain_ref.shape[0]
    seqs = lens_ref.shape[1]
    batch = nd * seqs
    rows = batch // nt
    dloc = gain_ref.shape[1]
    width = wx.shape[2]
    lgroups = width // WIDTH_X

    pairs = ((wdt_hbm, wdt), (wx_hbm, wx), (wb_hbm, wb), (wc_hbm, wc), (wz_hbm, wz), (wo_hbm, wo))

    def weight(layer, at):
        src, dst = pairs[at]
        return pltpu.make_async_copy(src.at[layer], dst.at[layer], w_sem.at[layer, at])

    def states(layer):
        return pltpu.make_async_copy(state_hbm.at[layer], state.at[layer], st_sem.at[layer])

    for at in range(5):
        weight(0, at).start()

    barrier = pltpu.get_barrier_semaphore()
    for k in range(1, nd):
        pl.semaphore_signal(
            barrier, inc=1, device_id={"dp": lax.rem(dp + k, nd)}, device_id_type=MESH
        )
    for k in range(1, nt):
        pl.semaphore_signal(
            barrier, inc=1, device_id={"tp": lax.rem(tp + k, nt)}, device_id_type=MESH
        )
    pl.semaphore_wait(barrier, nd - 1 + nt - 1)

    def scatter(layer, snd, rcv, at):
        copies = []
        for k in range(1, nd):
            peer = lax.rem(dp + k, nd)
            copy = pltpu.make_async_remote_copy(
                src_ref=snd.at[layer, peer],
                dst_ref=rcv.at[layer, k - 1],
                send_sem=dps.at[layer, at, k - 1],
                recv_sem=dpr.at[layer, at, k - 1],
                device_id={"dp": peer},
                device_id_type=MESH,
            )
            copy.start()
            copies.append(copy)
        return copies

    def gathered(copies, layer, snd, rcv):
        for copy in copies:
            copy.wait_recv()
        total = snd[layer, dp].astype(F32)
        for k in range(nd - 1):
            total = total + rcv[layer, k].astype(F32)
        return total

    heads_all = wdt.shape[1]
    lheads = bias_ref.shape[1]

    def expand(values, offset):
        count = values.shape[1]
        head = lax.broadcasted_iota(jnp.int32, (count, width), 0)
        lane = lax.broadcasted_iota(jnp.int32, (count, width), 1)
        pick = jnp.where(head == lane // HEAD_DIM + offset, 1.0, 0.0).astype(F32)
        return jnp.dot(
            values, pick, preferred_element_type=F32, precision=lax.Precision.HIGHEST
        )

    bias = expand(bias_ref[...], 0)
    rate = jnp.exp(expand(alog_ref[...], 0))
    skip = expand(skip_ref[...], 0)
    spread = jnp.broadcast_to(lens_ref[...].astype(F32), (seqs, seqs))
    diagonal = lax.broadcasted_iota(jnp.int32, (seqs, seqs), 0) == lax.broadcasted_iota(
        jnp.int32, (seqs, seqs), 1
    )
    lens = jnp.sum(jnp.where(diagonal, spread, 0.0), axis=1, keepdims=True)
    pending = []

    for layer in range(layers):
        source = tokens_ref if layer == 0 else stream.at[layer - 1]
        wide = source[...].astype(F32).reshape(batch, dloc)
        squares = jnp.sum(wide * wide, axis=-1, keepdims=True)
        normed_s[...] = (wide * gain_ref[layer : layer + 1, :]).astype(BF16)

        def project(w_ref, snd, layer=layer):
            n = w_ref.shape[2]
            tile = min(n, 256)

            def step(j, carry):
                cols = pl.ds(pl.multiple_of(j * tile, tile), tile)
                part = jnp.dot(
                    normed_s[...], w_ref[layer, :, cols], preferred_element_type=F32
                )
                snd[layer, :, :, cols] = part.reshape(nd, seqs, tile).astype(snd.dtype)
                return carry

            lax.fori_loop(0, n // tile, step, 0)

        weight(layer, 0).wait()
        part_dt = lax.dot_general(
            normed_s[...], wdt[layer], (((1,), (1,)), ((), ())), preferred_element_type=F32
        )
        snd_e[layer, :, :, 0:128] = jnp.zeros((nd, seqs, 128), F32)
        snd_e[layer, :, :, 0:heads_all] = part_dt.reshape(nd, seqs, heads_all)
        snd_e[layer, :, :, 128:256] = jnp.broadcast_to(squares, (batch, 128)).reshape(
            nd, seqs, 128
        )
        weight(layer, 1).wait()
        project(wx, snd_x)
        copies_x = scatter(layer, snd_x, rcv_x, 1)
        copies_e = scatter(layer, snd_e, rcv_e, 0)
        weight(layer, 2).wait()
        project(wb, snd_b)
        copies_b = scatter(layer, snd_b, rcv_b, 2)
        weight(layer, 3).wait()
        project(wc, snd_c)
        copies_c = scatter(layer, snd_c, rcv_c, 3)
        weight(layer, 4).wait()
        if layer == 0:
            states(0).start()
            weight(0, 5).start()
        project(wz, snd_z)
        copies_z = scatter(layer, snd_z, rcv_z, 4)
        if layer + 1 < layers:
            for at in range(6):
                weight(layer + 1, at).start()
            states(layer + 1).start()

        extra = gathered(copies_e, layer, snd_e, rcv_e)
        inverse = lax.rsqrt(extra[:, 128:129] / D + EPSILON)
        raw = expand(extra[:, 0:heads_all] * inverse, tp * lheads)
        softin = raw + bias[layer : layer + 1, :]
        step = jnp.maximum(softin, 0.0) + jnp.log1p(jnp.exp(-jnp.abs(softin)))
        decay = jnp.exp(-rate[layer : layer + 1, :] * step)
        decay = jnp.where(lens >= 2, decay, 0.0)

        values = (gathered(copies_x, layer, snd_x, rcv_x) * inverse).astype(BF16)
        writes = (gathered(copies_b, layer, snd_b, rcv_b) * inverse).astype(BF16)
        reads = (gathered(copies_c, layer, snd_c, rcv_c) * inverse).astype(BF16)
        pieces = []
        for g in range(lgroups):
            pieces.append(values[:, g * WIDTH_X : (g + 1) * WIDTH_X])
            pieces.append(writes[:, g * STATE : (g + 1) * STATE])
            pieces.append(reads[:, g * STATE : (g + 1) * STATE])
        current = jnp.concatenate(pieces, axis=1)
        cur_ref[layer] = current
        summed = current.astype(F32) * taps_ref[
            layer, CONV_W - 1 : CONV_W, :
        ].astype(F32)
        for tap in range(CONV_W - 1):
            past = conv_ref[layer, tap].astype(F32)
            past = jnp.where(lens >= CONV_W - tap, past, 0.0)
            if tap >= 1:
                kept_ref[layer, tap - 1] = past.astype(BF16)
            summed = summed + past * taps_ref[layer, tap : tap + 1, :].astype(F32)
        active = silu(summed)
        head_in = jnp.concatenate(
            [active[:, g * GROUP_W : g * GROUP_W + WIDTH_X] for g in range(lgroups)], axis=1
        )
        wk = [
            active[:, g * GROUP_W + WIDTH_X : g * GROUP_W + WIDTH_X + STATE]
            for g in range(lgroups)
        ]
        rk = [active[:, g * GROUP_W + WIDTH_X + STATE : (g + 1) * GROUP_W] for g in range(lgroups)]
        stepx = step * head_in
        dec_ref[layer] = decay
        sx_ref[layer] = stepx
        wk_ref[layer] = jnp.concatenate(wk, axis=1)
        rk_s[...] = jnp.concatenate(rk, axis=1)

        states(layer).wait()

        def read_eight(b, carry, layer=layer):
            at = pl.ds(pl.multiple_of(b * 8, 8), 8)
            keys = rk_s[at, :]
            lines = []
            for i in range(8):
                outs = []
                for g in range(lgroups):
                    row = keys[i : i + 1, g * STATE : (g + 1) * STATE]
                    lhs = jnp.broadcast_to(row, (16, STATE)).astype(BF16)
                    held = state[layer, b * 8 + i, g * PER_GROUP : (g + 1) * PER_GROUP]
                    held = held.reshape(WIDTH_X, STATE).astype(BF16)
                    res = lax.dot_general(
                        lhs, held, (((1,), (1,)), ((), ())), preferred_element_type=F32
                    )
                    outs.append(res[0:1])
                lines.append(jnp.concatenate(outs, axis=1))
            y_s[at, :] = jnp.concatenate(lines, axis=0)
            return carry

        lax.fori_loop(0, seqs // 8, read_eight, 0)
        readout = decay * y_s[...] + skip[layer : layer + 1, :] * head_in
        gate = (gathered(copies_z, layer, snd_z, rcv_z) * inverse).astype(BF16).astype(F32)
        gate = silu(gate)
        mixed = []
        for g in range(lgroups):
            cols = slice(g * WIDTH_X, (g + 1) * WIDTH_X)
            cross = jnp.sum(wk[g] * rk[g], axis=-1, keepdims=True)
            gated = (readout[:, cols] + stepx[:, cols] * cross) * gate[:, cols]
            norm = lax.rsqrt(jnp.mean(gated * gated, axis=-1, keepdims=True) + EPSILON)
            mixed.append(gated * norm * ogain_ref[layer : layer + 1, cols])
        mixes[layer, dp] = jnp.concatenate(mixed, axis=1).astype(BF16)
        copies_m = []
        for k in range(1, nd):
            copy = pltpu.make_async_remote_copy(
                src_ref=mixes.at[layer, dp],
                dst_ref=mixes.at[layer, dp],
                send_sem=ags.at[layer, k - 1],
                recv_sem=agr.at[layer, k - 1],
                device_id={"dp": lax.rem(dp + k, nd)},
                device_id_type=MESH,
            )
            copy.start()
            copies_m.append(copy)
        weight(layer, 5).wait()
        for copy in copies_m:
            copy.wait_recv()

        tile = min(dloc, 256)

        def project_out(j, carry, layer=layer):
            cols = pl.ds(pl.multiple_of(j * tile, tile), tile)
            lhs = mixes[layer].reshape(batch, width)
            part = jnp.dot(lhs, wo[layer, :, cols], preferred_element_type=F32)
            snd_o[layer, :, :, cols] = part.reshape(nt, rows, tile).astype(BF16)
            return carry

        lax.fori_loop(0, dloc // tile, project_out, 0)
        copies_o = []
        for k in range(1, nt):
            peer = lax.rem(tp + k, nt)
            copy = pltpu.make_async_remote_copy(
                src_ref=snd_o.at[layer, peer],
                dst_ref=rcv_o.at[layer, k - 1],
                send_sem=rss.at[layer, k - 1],
                recv_sem=rsr.at[layer, k - 1],
                device_id={"tp": peer},
                device_id_type=MESH,
            )
            copy.start()
            copies_o.append(copy)
        total = source[tp].astype(F32) + snd_o[layer, tp].astype(F32)
        for k in range(nt - 1):
            copies_o[k].wait_recv()
            total = total + rcv_o[layer, k].astype(F32)
        stream[layer, tp] = total.astype(BF16)
        copies_s = []
        for k in range(1, nt):
            copy = pltpu.make_async_remote_copy(
                src_ref=stream.at[layer, tp],
                dst_ref=stream.at[layer, tp],
                send_sem=tgs.at[layer, k - 1],
                recv_sem=tgr.at[layer, k - 1],
                device_id={"tp": lax.rem(tp + k, nt)},
                device_id_type=MESH,
            )
            copy.start()
            copies_s.append(copy)
        for copy in copies_s:
            copy.wait_recv()
        for group in (copies_e, copies_x, copies_b, copies_c, copies_z, copies_m, copies_o, copies_s):
            pending.extend(group)

    out_ref[...] = stream[layers - 1]
    for copy in pending:
        copy.wait_send()


def state_kernel(
    stream_ref, cur_ref, kept_ref, dec_ref, sx_ref, wk_ref, state_ref, out_ref, conv_ref, new_ref
):
    @pl.when(jnp.logical_and(pl.program_id(0) == 0, pl.program_id(1) == 0))
    def small():
        out_ref[...] = stream_ref[...]
        conv_ref[:, 0 : CONV_W - 2] = kept_ref[...]
        conv_ref[:, CONV_W - 2] = cur_ref[...]

    count = state_ref.shape[1]
    first = pl.program_id(1) * count
    width = dec_ref.shape[2]
    at = pl.ds(pl.multiple_of(first // 8 * 8, 8), 8)
    layer = pl.program_id(0)
    place = lax.rem(first, 8)

    def rows_of(ref):
        block = ref[layer, at, :]
        rows = block[0:count]
        for j in range(count, 8, count):
            rows = jnp.where(place == j, block[j : j + count], rows)
        return rows

    decs, sxs, wks = rows_of(dec_ref), rows_of(sx_ref), rows_of(wk_ref)
    for i in range(count):
        dec = jnp.broadcast_to(decs[i : i + 1], (64, width))
        sx = jnp.broadcast_to(sxs[i : i + 1], (64, width))
        cols = jnp.concatenate([dec, sx], axis=0).T
        for g in range(width // WIDTH_X):
            part = cols[g * WIDTH_X : (g + 1) * WIDTH_X]
            held = state_ref[0, i, g * PER_GROUP : (g + 1) * PER_GROUP].reshape(WIDTH_X, STATE)
            write = wks[i : i + 1, g * STATE : (g + 1) * STATE]
            new = part[:, 0:1] * held + part[:, 64:65] * write
            new_ref[0, i, g * PER_GROUP : (g + 1) * PER_GROUP] = new.reshape(
                PER_GROUP, HEAD_DIM, STATE
            )


def body(
    nd, nt,
    tokens, lengths, norm_gain, w_z, w_x, w_b, w_c, w_dt, conv_weight,
    dt_bias, a_log, d_skip, out_gain, w_out, conv_state, ssm_state,
):
    layers = w_z.shape[0]
    batch, dloc = tokens.shape
    seqs = lengths.shape[0]
    rows = batch // nt
    width = w_x.shape[2]
    keys = w_b.shape[2]
    turned = jnp.swapaxes(w_dt, 1, 2)
    conv_w = conv_weight.shape[2]
    vmem = pl.BlockSpec(memory_space=pltpu.VMEM)
    anywhere = pl.BlockSpec(memory_space=pl.ANY)
    dma = pltpu.SemaphoreType.DMA
    sizes = (width, keys, keys, width)
    stream, current, kept, dec, sx, wk = pl.pallas_call(
        functools.partial(block_kernel, nd, nt),
        out_shape=(
            jax.ShapeDtypeStruct((nt, rows, dloc), BF16),
            jax.ShapeDtypeStruct((layers, seqs, conv_w), BF16),
            jax.ShapeDtypeStruct((layers, CONV_W - 2, seqs, conv_w), BF16),
            jax.ShapeDtypeStruct((layers, seqs, width), F32),
            jax.ShapeDtypeStruct((layers, seqs, width), F32),
            jax.ShapeDtypeStruct((layers, seqs, keys), F32),
        ),
        in_specs=[vmem] * 9 + [anywhere] * 7,
        out_specs=[vmem] * 6,
        scratch_shapes=[
            pltpu.VMEM(w_z.shape, BF16),
            pltpu.VMEM(w_x.shape, BF16),
            pltpu.VMEM(w_b.shape, BF16),
            pltpu.VMEM(w_c.shape, BF16),
            pltpu.VMEM(turned.shape, BF16),
            pltpu.VMEM(w_out.shape, BF16),
            pltpu.VMEM(ssm_state.shape, F32),
            pltpu.VMEM((layers, nd, seqs, 256), F32),
            *[pltpu.VMEM((layers, nd, seqs, n), BF16) for n in sizes],
            pltpu.VMEM((layers, nd - 1, seqs, 256), F32),
            *[pltpu.VMEM((layers, nd - 1, seqs, n), BF16) for n in sizes],
            pltpu.VMEM((layers, nd, seqs, width), BF16),
            pltpu.VMEM((layers, nt, rows, dloc), BF16),
            pltpu.VMEM((layers, nt - 1, rows, dloc), BF16),
            pltpu.VMEM((layers, nt, rows, dloc), BF16),
            pltpu.VMEM((batch, dloc), BF16),
            pltpu.VMEM((seqs, keys), F32),
            pltpu.VMEM((seqs, width), F32),
            dma((layers, 6)),
            dma((layers,)),
            dma((layers, 5, nd - 1)),
            dma((layers, 5, nd - 1)),
            dma((layers, nd - 1)),
            dma((layers, nd - 1)),
            dma((layers, nt - 1)),
            dma((layers, nt - 1)),
            dma((layers, nt - 1)),
            dma((layers, nt - 1)),
        ],
        compiler_params=pltpu.CompilerParams(
            collective_id=0, has_side_effects=True, vmem_limit_bytes=56 * 1024 * 1024
        ),
    )(
        tokens.reshape(nt, rows, dloc), lengths[None, :], norm_gain, dt_bias, a_log, d_skip,
        out_gain, conv_weight, jnp.transpose(conv_state, (0, 2, 1, 3)),
        w_z, w_x, w_b, w_c, turned, w_out, ssm_state,
    )
    step = 2
    block = (1, step) + ssm_state.shape[2:]
    mixed_out, conv_new, ssm_new = pl.pallas_call(
        state_kernel,
        grid=(layers, seqs // step),
        out_shape=(
            jax.ShapeDtypeStruct(stream.shape, BF16),
            jax.ShapeDtypeStruct((layers, CONV_W - 1, seqs, conv_w), BF16),
            jax.ShapeDtypeStruct(ssm_state.shape, F32),
        ),
        in_specs=[vmem] * 6 + [pl.BlockSpec(block, lambda l, s: (l, s, 0, 0, 0))],
        out_specs=(vmem, vmem, pl.BlockSpec(block, lambda l, s: (l, s, 0, 0, 0))),
    )(stream, current, kept, dec, sx, wk, ssm_state)
    return mixed_out.reshape(batch, dloc), jnp.transpose(conv_new, (0, 2, 1, 3)), ssm_new


def solution(mesh):
    placed = (
        P("grp", "dp"),
        P(("grp", "dp")),
        P(None, "dp"),
        P(None, "dp", "tp"),
        P(None, "dp", "tp"),
        P(None, "dp", "tp"),
        P(None, "dp", "tp"),
        P(None, "dp", None),
        P(None, None, "tp"),
        P(None, "tp"),
        P(None, "tp"),
        P(None, "tp"),
        P(None, "tp"),
        P(None, "tp", "dp"),
        P(None, ("grp", "dp"), None, "tp"),
        P(None, ("grp", "dp"), "tp", None, None),
    )
    return jax.shard_map(
        functools.partial(body, mesh.shape["dp"], mesh.shape["tp"]),
        mesh=mesh,
        in_specs=placed,
        out_specs=(
            P("grp", "dp"),
            P(None, ("grp", "dp"), None, "tp"),
            P(None, ("grp", "dp"), "tp", None, None),
        ),
        check_vma=False,
    )
```
